512 devices in a mesh: ep: 32 (over z, core), tp: 16 (over y, x).
Axes of the slice: x: 4, y: 4, z: 16, core: 2. Of those that a mesh axis runs over, the one named last changes fastest.
Arguments:
- mixer_value_input: bfloat16 [8192, 4096], P('ep', 'tp'), may hold values from -6 to 6
- input_state_matrix: bfloat16 [8192, 2048], P('ep', 'tp'), may hold values from -6 to 6
- output_state_matrix: bfloat16 [8192, 2048], P('ep', 'tp'), may hold values from -6 to 6
- output_gate_input: bfloat16 [8192, 4096], P('ep', 'tp'), may hold values from -6 to 6
- step_input: float32 [8192, 64], P('ep', 'tp'), may hold values from -6 to -2
- extra_log_decay: float32 [8192, 64], P('ep', 'tp'), may hold values from -1 to 0
- head_log_decay: float32 [64], P('tp'), may hold values from -10 to 1
- head_skip_scale: float32 [64], P('tp'), may hold values from 0.5 to 2
- value_kernel: float32 [4, 4096], P(None, 'tp'), may hold values from -3 to 3
- input_matrix_kernel: float32 [4, 2048], P(None, 'tp'), may hold values from -3 to 3
- output_matrix_kernel: float32 [4, 2048], P(None, 'tp'), may hold values from -3 to 3
- mixer_norm_scale: float32 [4096], P('tp'), may hold values from 0.1 to 1.9
- mixer_output_weight: bfloat16 [4096, 2048], P(None, 'tp'), may hold values from -0.09375 to 0.09375
- second_token_rows: bfloat16 [8192, 2048], P('ep'), may hold values from -6 to 6
- expert_norm_scale: float32 [2048], replicated, may hold values from 0.1 to 1.9
- routed_expert_index: int32 [8192, 4], P('ep'), may hold values from 0 to 63, all different within a row; in each aligned block of 256 rows (0 to 255, 256 to 511, ...) at most 24 rows name the same one
- routed_expert_weight: float32 [8192, 4], P('ep'), may hold values from 0.1 to 1
- routed_gate_weight: bfloat16 [64, 2048, 1024], P('ep', None, 'tp'), may hold values from -0.125 to 0.125
- routed_up_weight: bfloat16 [64, 2048, 1024], P('ep', None, 'tp'), may hold values from -0.125 to 0.125
- routed_down_weight: bfloat16 [64, 1024, 2048], P('ep', None, 'tp'), may hold values from -0.1875 to 0.1875
- shared_gate_weight: bfloat16 [2048, 1024], P(None, 'tp'), may hold values from -0.125 to 0.125
- shared_up_weight: bfloat16 [2048, 1024], P(None, 'tp'), may hold values from -0.125 to 0.125
- shared_down_weight: bfloat16 [1024, 2048], P(None, 'tp'), may hold values from -0.1875 to 0.1875
Outputs:
- mixer_output: bfloat16 [8192, 2048], P('ep', 'tp')
- routed_out: bfloat16 [8192, 2048], P('ep', 'tp')
The draws below stay inside these ranges and needn't reach their ends.
Inputs may be any that keep to these rules, and one draw needn't show every extreme that they name: `routed_expert_index`: in each aligned block of 256 rows (the rows of one index of ep) no expert is named more than 24 times, a bound that some block reaches.
All inputs are finite; a program needn't handle non-finite values.
Results may differ from the reference program's by a relative error of at most 0.012.
Values may be sent and summed in bfloat16 or wider, within the bound.
No kernel may reach another device: no remote copies, remote signals or barrier semaphores. Data moves between devices by JAX's collectives and lax.ppermute only.
A program may use at most 64 MiB of HBM per device.

```python
import math
from functools import partial
import jax
import jax.numpy as jnp
import numpy as np
from jax import lax

D = 2048
HEADS = 64
HEAD_DIM = 64
INNER = 4096
GROUPS = 16
STATE = 128
CONV_TAPS = 4
BLOCK = 128
EXPERT_FF = 1024
SHARED_FF = 1024
EXPERTS = 64
TOP_K = 4
TOK_B = 256
TOKENS_A = 8192
TOKENS_B = 8192
CAP = 24
N_EP = 32


def draw_step_input(key, part):
    first_key, second_key = jax.random.split(jax.random.fold_in(key, 11))
    nblocks = TOKENS_A // BLOCK
    offset = jax.random.uniform(first_key, (nblocks, 1, HEADS), jnp.float32, -0.7, 0.7)
    noise = 0.3 * jax.random.truncated_normal(second_key, -2.0, 2.0, (nblocks, BLOCK, HEADS), jnp.float32)
    return (-4.0 + offset + noise).reshape(TOKENS_A, HEADS)


def draw_extra_log_decay(key, part):
    first_key, second_key = jax.random.split(jax.random.fold_in(key, 23))
    spots = jax.random.randint(first_key, (2,), 0, TOKENS_A)
    positions = jnp.arange(TOKENS_A)
    struck = jnp.any(positions[:, None] == spots[None, :], axis=1)
    losses = jnp.log(jax.random.uniform(second_key, (TOKENS_A, HEADS), jnp.float32, 0.5, 0.8))
    return jnp.where(struck[:, None], losses, 0.0).astype(jnp.float32)


def draw_head_log_decay(key, part):
    first_key, second_key, third_key = jax.random.split(jax.random.fold_in(key, 37), 3)
    slow_share = 0.5
    slow_heads = jax.random.uniform(first_key, (HEADS,), jnp.float32) < slow_share
    slow_rate = jax.random.uniform(second_key, (HEADS,), jnp.float32, 0.2, 1.0) * 30.0 / TOKENS_A
    fast_rate = jnp.exp(jax.random.uniform(third_key, (HEADS,), jnp.float32, jnp.log(0.5), jnp.log(1.5)))
    return jnp.log(jnp.where(slow_heads, slow_rate, fast_rate)).astype(jnp.float32)


def shard_levels(key, dims, shards, smallest, top_value):
    def one(axis_at, blocks):
        heights = jax.random.uniform(jax.random.fold_in(jax.random.fold_in(key, 6), axis_at), (blocks,), jnp.float32, smallest / len(shards), top_value / len(shards))
        return jnp.repeat(jnp.exp(heights), dims[axis_at] // blocks).reshape((-1,) + (1,) * (len(dims) - axis_at - 1))

    level = one(*shards[0])
    for cut in shards[1:]:
        level = level * one(*cut)
    return level


def deal_out(rng, own, number, rows, count, top, limit, lean):
    sequence = jax.random.permutation(rng, count)
    packed, common = portions_of(count, rows * top, limit, lean, True), portions_of(count, rows * top, limit, lean, False)
    places = jnp.arange(count)

    def named(tallies, turn):
        used = int((tallies > 0).sum())
        fixed = max(1, used // 4)
        moved = fixed + (places - fixed + turn * (used - fixed)) % max(1, count - fixed)
        return jnp.zeros((count,), jnp.int32).at[sequence[jnp.where(places < fixed, places, moved)]].set(jnp.asarray(tallies, jnp.int32))

    tallies = jnp.where(number % 4 == 0, named(packed, number // 4), named(common, number - number // 4 - 1))
    mixed = jax.random.permutation(jax.random.fold_in(own, 3), count)
    donor, sink = mixed[0:count // 2 * 2:2], mixed[1:count // 2 * 2:2]
    slack = jnp.minimum(tallies[donor] - 1, limit - tallies[sink]) // 2
    slack = jnp.where((donor == sequence[0]) | (sink == sequence[0]) | (tallies[sink] == 0), 0, jnp.maximum(slack, 0))
    moved = jax.random.randint(jax.random.fold_in(own, 4), (count // 2,), 0, 1 << 20) % (slack + 1)
    tallies = tallies.at[donor].add(-moved).at[sink].add(moved)
    labels = jnp.searchsorted(jnp.cumsum(tallies), jnp.arange(rows * top), side="right").astype(jnp.int32)
    table = labels.reshape(top, rows).T
    table = table[jax.random.permutation(jax.random.fold_in(own, 1), rows)]
    turn = jax.random.randint(jax.random.fold_in(own, 2), (rows, 1), 0, top)
    return jnp.take_along_axis(table, (jnp.arange(top)[None, :] + turn) % top, axis=1)


def portions_of(amount, total, bound, skew, full):
    weights = [(1 << 20) // math.isqrt(grade ** skew) + 1 for grade in range(1, amount + 1)]
    largest = bound if full else min(bound, max(-(-total // amount), total * weights[0] // sum(weights)))
    least = 1 if total - largest >= amount - 1 else 0
    counts, spare = [largest] + [least] * (amount - 1), total - largest - least * (amount - 1)
    while spare > 0:
        candidates = [i for i in range(1, amount) if counts[i] < largest] or [i for i in range(1, amount) if counts[i] < bound]
        whole, remaining = sum([weights[i] for i in candidates]), spare
        for i in candidates:
            extra = min(bound - counts[i], max(1, remaining * weights[i] // whole), spare)
            counts[i] = counts[i] + extra
            spare = spare - extra
    return np.array(counts)


def gaussian(key, shape, width, most, cuts=(), kind=jnp.bfloat16):
    array = jax.random.normal(key, shape, jnp.float32) * width
    if len(cuts) > 0:
        array = shard_levels(key, shape, cuts, -0.22, 0.18) * array
    return jnp.clip(array, min=-most, max=most).astype(kind)


def setup_inputs(seed: int = 0) -> dict:
    arg_keys = jax.random.split(jax.random.key(seed), 24)
    mixer_value_input = gaussian(arg_keys[0], (TOKENS_A, INNER), 1.0, 6.0, ((0, 32), (1, 16)))
    input_state_matrix = gaussian(arg_keys[1], (TOKENS_A, GROUPS * STATE), 1.0, 6.0, ((0, 32), (1, 16)))
    output_state_matrix = gaussian(arg_keys[2], (TOKENS_A, GROUPS * STATE), 1.0, 6.0, ((0, 32), (1, 16)))
    output_gate_input = gaussian(arg_keys[3], (TOKENS_A, INNER), 1.0, 6.0, ((0, 32), (1, 16)))
    step_input = draw_step_input(jax.random.fold_in(arg_keys[23], 71), 0)
    extra_log_decay = draw_extra_log_decay(jax.random.fold_in(arg_keys[23], 71), 0)
    head_log_decay = draw_head_log_decay(jax.random.fold_in(arg_keys[23], 71), 0)
    head_skip_scale = jnp.clip(0.5 + 1.5 * jax.random.uniform(arg_keys[7], (HEADS,), jnp.float32) ** shard_levels(arg_keys[7], (HEADS,), ((0, 16),), -0.2, 0.2), 0.5, 2.0)
    value_kernel = gaussian(arg_keys[8], (CONV_TAPS, INNER), 0.5, 3.0, ((1, 16),), jnp.float32)
    input_matrix_kernel = gaussian(arg_keys[9], (CONV_TAPS, GROUPS * STATE), 0.5, 3.0, ((1, 16),), jnp.float32)
    output_matrix_kernel = gaussian(arg_keys[10], (CONV_TAPS, GROUPS * STATE), 0.5, 3.0, ((1, 16),), jnp.float32)
    mixer_norm_scale = jnp.clip(1.0 + 0.18 * jax.random.normal(arg_keys[11], (INNER,), jnp.float32), 0.1, 1.9)
    mixer_output_weight = gaussian(arg_keys[12], (INNER, D), INNER ** -0.5, 0.09375, ((1, 16),))
    second_token_rows = gaussian(arg_keys[13], (TOKENS_B, D), 1.0, 6.0, ((0, 32),))
    expert_norm_scale = jnp.clip(1.0 + 0.18 * jax.random.normal(arg_keys[14], (D,), jnp.float32), 0.1, 1.9)
    routed_expert_index_keys = jax.random.split(jax.random.fold_in(arg_keys[15], 1), TOKENS_B // TOK_B)
    routed_expert_index_turns = jax.random.permutation(jax.random.fold_in(arg_keys[15], 3), TOKENS_B // TOK_B)
    routed_expert_index = jax.vmap(lambda own, number: deal_out(jax.random.fold_in(arg_keys[15], 2), own, number, TOK_B, EXPERTS, TOP_K, CAP, 2))(routed_expert_index_keys, routed_expert_index_turns).reshape((TOKENS_B, TOP_K))
    routed_expert_weight = jnp.clip(0.1 + 0.9 * jax.random.uniform(arg_keys[16], (TOKENS_B, TOP_K), jnp.float32) ** shard_levels(arg_keys[16], (TOKENS_B, TOP_K), ((0, 32),), -0.2, 0.2), 0.1, 1.0)
    routed_gate_weight = gaussian(arg_keys[17], (EXPERTS, D, EXPERT_FF), D ** -0.5, 0.125, ((0, 32), (2, 16)))
    routed_up_weight = gaussian(arg_keys[18], (EXPERTS, D, EXPERT_FF), D ** -0.5, 0.125, ((0, 32), (2, 16)))
    routed_down_weight = gaussian(arg_keys[19], (EXPERTS, EXPERT_FF, D), EXPERT_FF ** -0.5, 0.1875, ((0, 32), (2, 16)))
    shared_gate_weight = gaussian(arg_keys[20], (D, SHARED_FF), D ** -0.5, 0.125, ((1, 16),))
    shared_up_weight = gaussian(arg_keys[21], (D, SHARED_FF), D ** -0.5, 0.125, ((1, 16),))
    shared_down_weight = gaussian(arg_keys[22], (SHARED_FF, D), SHARED_FF ** -0.5, 0.1875, ((1, 16),))
    return {"mixer_value_input": mixer_value_input, "input_state_matrix": input_state_matrix, "output_state_matrix": output_state_matrix, "output_gate_input": output_gate_input, "step_input": step_input, "extra_log_decay": extra_log_decay, "head_log_decay": head_log_decay, "head_skip_scale": head_skip_scale, "value_kernel": value_kernel, "input_matrix_kernel": input_matrix_kernel, "output_matrix_kernel": output_matrix_kernel, "mixer_norm_scale": mixer_norm_scale, "mixer_output_weight": mixer_output_weight, "second_token_rows": second_token_rows, "expert_norm_scale": expert_norm_scale, "routed_expert_index": routed_expert_index, "routed_expert_weight": routed_expert_weight, "routed_gate_weight": routed_gate_weight, "routed_up_weight": routed_up_weight, "routed_down_weight": routed_down_weight, "shared_gate_weight": shared_gate_weight, "shared_up_weight": shared_up_weight, "shared_down_weight": shared_down_weight}


epsilon = 1e-05
precise = lax.Precision.HIGHEST

def conv_silu(source, weights):
    length = source.shape[0]
    padded = jnp.concatenate([jnp.zeros((CONV_TAPS - 1, source.shape[1]), source.dtype), source], axis=0)
    total_sum = jnp.zeros(source.shape, jnp.float32)
    for tap_index in range(CONV_TAPS):
        total_sum = total_sum + padded[tap_index:tap_index + length].astype(jnp.float32) * weights[tap_index]
    return jax.nn.silu(total_sum).astype(jnp.bfloat16)

def route_slots(route_block, experts, capacity):
    flat_ids = route_block.reshape(-1)
    onehot = (flat_ids[:, None] == jnp.arange(experts, dtype=jnp.int32)[None, :]).astype(jnp.int32)
    earlier = jnp.cumsum(onehot, axis=0) - onehot
    position_in = lax.optimization_barrier(jnp.sum(earlier * onehot, axis=1)).astype(jnp.int32)
    slot_index = (flat_ids * capacity + position_in).astype(jnp.int32)
    owner_row = (jnp.arange(flat_ids.shape[0], dtype=jnp.int32) // route_block.shape[1]).astype(jnp.int32)
    slot_owner = jnp.full((experts * capacity,), route_block.shape[0], jnp.int32).at[slot_index].set(owner_row)
    return (slot_owner, slot_index)

def spread_weights(slot_index, weights, count):
    return jnp.zeros((count,), jnp.float32).at[slot_index].set(weights)

def mixer_portion(mixer_value_input, input_state_matrix, output_state_matrix, output_gate_input, step_input, extra_log_decay, head_log_decay, head_skip_scale, value_kernel, input_matrix_kernel, output_matrix_kernel, mixer_norm_scale, mixer_output_weight):
    length = mixer_value_input.shape[0]
    values = conv_silu(mixer_value_input, value_kernel)
    in_mat = conv_silu(input_state_matrix, input_matrix_kernel)
    out_mat = conv_silu(output_state_matrix, output_matrix_kernel)
    step_length = jax.nn.softplus(step_input)
    decay_logarithm = -jnp.exp(head_log_decay)[None, :] * step_length + extra_log_decay
    head_ratio = HEADS // GROUPS
    nblocks = length // BLOCK
    value_wide = values.astype(jnp.float32).reshape(nblocks, BLOCK, HEADS, HEAD_DIM)
    in_wide = in_mat.astype(jnp.float32).reshape(nblocks, BLOCK, GROUPS, STATE)
    out_wide = out_mat.astype(jnp.float32).reshape(nblocks, BLOCK, GROUPS, STATE)
    step_blocks = step_length.reshape(nblocks, BLOCK, HEADS)
    log_blocks = decay_logarithm.reshape(nblocks, BLOCK, HEADS)
    lower_mask = jnp.tril(jnp.ones((BLOCK, BLOCK), bool))

    def advance(carried, inputs):
        value_blk, in_blk, out_blk, step_blk, log_blk = inputs
        running = jnp.cumsum(log_blk, axis=0)
        scaled = value_blk * step_blk[:, :, None]
        scores = jnp.einsum('ign,jgn->gij', out_blk, in_blk, precision=precise)
        scores = jnp.repeat(scores, head_ratio, axis=0)
        spread = jnp.transpose(running[:, None, :] - running[None, :, :], (2, 0, 1))
        decay_mat = jnp.where(lower_mask[None], jnp.exp(jnp.where(lower_mask[None], spread, 0.0)), 0.0)
        inside = jnp.einsum('hij,jhp->ihp', scores * decay_mat, scaled, precision=precise)
        out_head = jnp.repeat(out_blk, head_ratio, axis=1)
        in_head = jnp.repeat(in_blk, head_ratio, axis=1)
        carried_term = jnp.einsum('ihn,hpn->ihp', out_head, carried, precision=precise) * jnp.exp(running)[:, :, None]
        to_end = jnp.exp(running[-1][None, :] - running)
        updated = carried * jnp.exp(running[-1])[:, None, None] + jnp.einsum('jhn,jh,jhp->hpn', in_head, to_end, scaled, precision=precise)
        return (updated, inside + carried_term)
    start_state = jnp.zeros((HEADS, HEAD_DIM, STATE), jnp.float32)
    _, mixed_heads = lax.scan(advance, start_state, (value_wide, in_wide, out_wide, step_blocks, log_blocks))
    mixed_heads = mixed_heads.reshape(length, HEADS, HEAD_DIM) + head_skip_scale[None, :, None] * value_wide.reshape(length, HEADS, HEAD_DIM)
    gated_heads = mixed_heads * jax.nn.silu(output_gate_input.astype(jnp.float32)).reshape(length, HEADS, HEAD_DIM)
    grouped = gated_heads.reshape(length, GROUPS, head_ratio * HEAD_DIM)
    grouped = grouped * lax.rsqrt(lax.optimization_barrier(jnp.mean(grouped * grouped, axis=-1, keepdims=True)) + epsilon)
    normed = (grouped.reshape(length, HEADS * HEAD_DIM) * mixer_norm_scale).astype(jnp.bfloat16)
    return jnp.dot(normed, mixer_output_weight, preferred_element_type=jnp.float32).astype(jnp.bfloat16)

def expert_part(second_token_rows, expert_norm_scale, routed_expert_index, routed_expert_weight, routed_gate_weight, routed_up_weight, routed_down_weight, shared_gate_weight, shared_up_weight, shared_down_weight):
    total_rows = second_token_rows.shape[0]
    rows_wide = second_token_rows.astype(jnp.float32)
    normed = (rows_wide * lax.rsqrt(lax.optimization_barrier(jnp.mean(rows_wide * rows_wide, axis=-1, keepdims=True)) + epsilon) * expert_norm_scale).astype(jnp.bfloat16)
    block_ids = routed_expert_index.reshape(N_EP, TOK_B, TOP_K)
    tables, slot_sets = jax.vmap(partial(route_slots, experts=EXPERTS, capacity=CAP))(block_ids)
    offsets = (jnp.arange(N_EP, dtype=jnp.int32) * TOK_B)[:, None]
    global_rows = jnp.where(tables == TOK_B, total_rows, tables + offsets).astype(jnp.int32)
    slot_weights = jax.vmap(partial(spread_weights, count=EXPERTS * CAP))(slot_sets, routed_expert_weight.reshape(N_EP, TOK_B * TOP_K))
    expert_rows = global_rows.reshape(N_EP, EXPERTS, CAP).transpose(1, 0, 2).reshape(EXPERTS, N_EP * CAP)
    expert_weights = slot_weights.reshape(N_EP, EXPERTS, CAP).transpose(1, 0, 2).reshape(EXPERTS, N_EP * CAP)
    padded = jnp.concatenate([normed, jnp.zeros((1, normed.shape[1]), jnp.bfloat16)], axis=0)

    def one_expert(accumulated, inputs):
        row_index, weights, gate_w, up_w, down_w = inputs
        picked = jnp.take(padded, row_index, axis=0)
        hidden = (jax.nn.silu(jnp.dot(picked, gate_w, preferred_element_type=jnp.float32)) * jnp.dot(picked, up_w, preferred_element_type=jnp.float32)).astype(jnp.bfloat16)
        output = jnp.dot(hidden, down_w, preferred_element_type=jnp.float32).astype(jnp.bfloat16)
        return (accumulated.at[row_index].add(output.astype(jnp.float32) * weights[:, None]), None)
    accumulated = jnp.zeros((total_rows + 1, normed.shape[1]), jnp.float32)
    accumulated, _ = lax.scan(one_expert, accumulated, (expert_rows, expert_weights, routed_gate_weight, routed_up_weight, routed_down_weight))
    shared_hidden = (jax.nn.silu(jnp.dot(normed, shared_gate_weight, preferred_element_type=jnp.float32)) * jnp.dot(normed, shared_up_weight, preferred_element_type=jnp.float32)).astype(jnp.bfloat16)
    shared_result = jnp.dot(shared_hidden, shared_down_weight, preferred_element_type=jnp.float32)
    return (accumulated[:total_rows] + shared_result).astype(jnp.bfloat16)

def reference(mixer_value_input, input_state_matrix, output_state_matrix, output_gate_input, step_input, extra_log_decay, head_log_decay, head_skip_scale, value_kernel, input_matrix_kernel, output_matrix_kernel, mixer_norm_scale, mixer_output_weight, second_token_rows, expert_norm_scale, routed_expert_index, routed_expert_weight, routed_gate_weight, routed_up_weight, routed_down_weight, shared_gate_weight, shared_up_weight, shared_down_weight):
    mixer_output = mixer_portion(mixer_value_input, input_state_matrix, output_state_matrix, output_gate_input, step_input, extra_log_decay, head_log_decay, head_skip_scale, value_kernel, input_matrix_kernel, output_matrix_kernel, mixer_norm_scale, mixer_output_weight)
    routed_out = expert_part(second_token_rows, expert_norm_scale, routed_expert_index, routed_expert_weight, routed_gate_weight, routed_up_weight, routed_down_weight, shared_gate_weight, shared_up_weight, shared_down_weight)
    return (mixer_output, routed_out)
```

```python
import jax
import jax.numpy as jnp
from jax import lax
from jax.sharding import PartitionSpec as P

HEAD_DIM = 64
STATE = 128
CONV_TAPS = 4
BLOCK = 128
TOP_K = 4
epsilon = 1e-05
F32 = jnp.float32
BF16 = jnp.bfloat16


def passed_along(x, axis, by):
    size = lax.axis_size(axis)
    pairs = [(i, i + by) for i in range(size) if 0 <= i + by < size]
    return lax.ppermute(x, axis, pairs)


def high(x):
    return lax.reduce_precision(x, 8, 7)


def three_parts(x):
    a = high(x)
    b = high(x - a)
    return a, b, x - a - b


def laid_out(tiles, dim):
    tiles = jnp.moveaxis(tiles, 0, dim)
    dims = tiles.shape
    return tiles.reshape(*dims[:dim], dims[dim] * dims[dim + 1], *dims[dim + 2 :])


def one_gather(arrays, axis, dims):
    ravelled = jnp.concatenate([a.reshape(-1) for a in arrays])
    lines, at, finished = (lax.all_gather(ravelled, axis), 0, [])
    for a, dim in zip(arrays, dims):
        tiles = lines[:, at : at + a.size].reshape(-1, *a.shape)
        finished.append(laid_out(tiles, dim))
        at += a.size
    return tuple(finished)


def conv_silu(tail_rows, source, weights):
    length = source.shape[0]
    padded = jnp.concatenate([tail_rows, source], axis=0)
    total_sum = jnp.zeros(source.shape, F32)
    for tap_index in range(CONV_TAPS):
        total_sum = (
            total_sum
            + padded[tap_index : tap_index + length].astype(F32) * weights[tap_index]
        )
    return jax.nn.silu(total_sum).astype(BF16)


def state_before(log_total, total_state):
    heads = log_total.shape[0]
    count = lax.axis_size("ep")
    place = lax.axis_index("ep")
    parts = jnp.stack(three_parts(log_total)).reshape(1, 3 * heads)
    row = jnp.pad(parts, ((0, 15), (0, STATE - 3 * heads)))
    rows = heads * HEAD_DIM
    payload = jnp.concatenate([total_state.reshape(rows, STATE), row], axis=0).astype(BF16)
    gathered = lax.all_gather(payload, "ep")
    tail = gathered[:, rows, : 3 * heads].astype(F32).reshape(count, 3, heads)
    logs = jnp.sum(tail, axis=1)
    at = jnp.arange(count)
    between = (at[None, :] > at[:, None]) & (at[None, :] < place)
    spans = jnp.sum(jnp.where(between[:, :, None], logs[None], 0.0), axis=1)
    weights = jnp.where((at < place)[:, None], jnp.exp(spans), 0.0)
    wide = jnp.repeat(weights, HEAD_DIM, axis=1)[:, :, None]
    summed = jnp.sum(gathered[:, :rows, :].astype(F32) * wide, axis=0)
    return summed.reshape(heads, HEAD_DIM, STATE)


def routes(index_t, weight_t, experts, capacity):
    rows = index_t.shape[1]
    ids = jnp.arange(experts, dtype=jnp.int32)[:, None]
    named = jnp.zeros((experts, rows), F32)
    weight = jnp.zeros((experts, rows), F32)
    for k in range(TOP_K):
        hit = index_t[k][None, :] == ids
        named = jnp.where(hit, 1.0, named)
        weight = jnp.where(hit, weight_t[k][None, :], weight)
    at = jnp.arange(rows)
    earlier = (at[:, None] < at[None, :]).astype(BF16)
    place = jnp.dot(named.astype(BF16), earlier, preferred_element_type=F32)
    place = jnp.where(named > 0.0, place, -1.0)
    slots = jnp.arange(capacity, dtype=jnp.int32).astype(F32)[None, :, None]
    taken = place[:, None, :] == slots
    return taken, weight


def on_device(
    mixer_value_input,
    input_state_matrix,
    output_state_matrix,
    output_gate_input,
    step_input,
    extra_log_decay,
    head_log_decay,
    head_skip_scale,
    value_kernel,
    input_matrix_kernel,
    output_matrix_kernel,
    mixer_norm_scale,
    mixer_output_weight,
    second_token_rows,
    expert_norm_scale,
    routed_expert_index,
    routed_expert_weight,
    routed_gate_weight,
    routed_up_weight,
    routed_down_weight,
    shared_gate_weight,
    shared_up_weight,
    shared_down_weight,
):
    length = mixer_value_input.shape[0]
    heads_local = step_input.shape[1]
    width_x = mixer_value_input.shape[1]
    width_b = input_state_matrix.shape[1]
    groups_local = width_b // STATE
    head_ratio = heads_local // groups_local
    nblocks = length // BLOCK
    lead_row = length - CONV_TAPS + 1
    edge_rows = jnp.concatenate(
        [
            mixer_value_input[lead_row:],
            input_state_matrix[lead_row:],
            output_state_matrix[lead_row:],
        ],
        axis=1,
    )
    tail_rows = passed_along(edge_rows, "ep", 1)
    values = conv_silu(tail_rows[:, :width_x], mixer_value_input, value_kernel)
    in_mat = conv_silu(
        tail_rows[:, width_x : width_x + width_b], input_state_matrix, input_matrix_kernel
    )
    out_mat = conv_silu(
        tail_rows[:, width_x + width_b :], output_state_matrix, output_matrix_kernel
    )
    step_length = jax.nn.softplus(step_input)
    decay_logarithm = -jnp.exp(head_log_decay)[None, :] * step_length + extra_log_decay
    running = jnp.cumsum(decay_logarithm.reshape(nblocks, BLOCK, heads_local), axis=1)
    value_wide = values.astype(F32).reshape(nblocks, BLOCK, heads_local, HEAD_DIM)
    scaled = value_wide * step_length.reshape(nblocks, BLOCK, heads_local)[..., None]
    in_blocks = in_mat.reshape(nblocks, BLOCK, groups_local, STATE)
    out_blocks = out_mat.reshape(nblocks, BLOCK, groups_local, STATE)
    scores = jnp.einsum("bign,bjgn->bgij", out_blocks, in_blocks, preferred_element_type=F32)
    scores = jnp.repeat(scores, head_ratio, axis=1)
    spread = jnp.transpose(running[:, :, None, :] - running[:, None, :, :], (0, 3, 1, 2))
    lower_mask = jnp.tril(jnp.ones((BLOCK, BLOCK), bool))[None, None]
    decay_mat = jnp.where(lower_mask, jnp.exp(jnp.where(lower_mask, spread, 0.0)), 0.0)
    inside = jnp.einsum("bhij,bjhp->bihp", scores * decay_mat, scaled)
    out_head = jnp.repeat(out_blocks.astype(F32), head_ratio, axis=2)
    in_head = jnp.repeat(in_blocks.astype(F32), head_ratio, axis=2)
    block_logs = running[:, -1]
    to_end = jnp.exp(block_logs[:, None, :] - running)
    block_state = jnp.einsum("bjhn,bjh,bjhp->bhpn", in_head, to_end, scaled)
    carried = jnp.zeros((heads_local, HEAD_DIM, STATE), F32)
    before = []
    for b in range(nblocks):
        before.append(carried)
        carried = carried * jnp.exp(block_logs[b])[:, None, None] + block_state[b]
    local_prev = jnp.stack(before)
    before_logs = jnp.cumsum(block_logs, axis=0) - block_logs
    incoming = state_before(jnp.sum(block_logs, axis=0), carried)
    entering = local_prev + jnp.exp(before_logs)[:, :, None, None] * incoming[None]
    carried_term = jnp.einsum("bihn,bhpn->bihp", out_head, entering) * jnp.exp(running)[..., None]
    mixed_heads = (inside + carried_term).reshape(length, heads_local, HEAD_DIM)
    mixed_heads = mixed_heads + head_skip_scale[None, :, None] * value_wide.reshape(
        length, heads_local, HEAD_DIM
    )
    gated_heads = mixed_heads * jax.nn.silu(output_gate_input.astype(F32)).reshape(
        length, heads_local, HEAD_DIM
    )
    grouped = gated_heads.reshape(length, groups_local, head_ratio * HEAD_DIM)
    grouped = grouped * lax.rsqrt(jnp.mean(grouped * grouped, axis=-1, keepdims=True) + epsilon)
    mixer_normed = (grouped.reshape(length, width_x) * mixer_norm_scale).astype(BF16)

    rows_local = second_token_rows.shape[0]
    model_width = second_token_rows.shape[1]
    local_experts = routed_gate_weight.shape[0]
    ep_count = lax.axis_size("ep")
    experts = local_experts * ep_count
    capacity = max(2, 3 * rows_local * TOP_K // (2 * experts))
    col_width = model_width // lax.axis_size("tp")
    rows_wide = second_token_rows.astype(F32)
    normed = (
        rows_wide
        * lax.rsqrt(jnp.mean(rows_wide * rows_wide, axis=-1, keepdims=True) + epsilon)
        * expert_norm_scale
    ).astype(BF16)
    taken, weight = routes(routed_expert_index.T, routed_expert_weight.T, experts, capacity)
    one_hot = taken.astype(BF16).reshape(experts * capacity, rows_local)
    mine = lax.dynamic_slice_in_dim(normed, lax.axis_index("tp") * col_width, col_width, 1)
    my_columns = jnp.dot(one_hot, mine, preferred_element_type=F32).astype(BF16)
    my_columns = my_columns.reshape(experts, capacity, col_width)
    arrived = lax.all_to_all(my_columns, "ep", split_axis=0, concat_axis=1, tiled=True)
    column_piece = lax.all_gather(arrived, "tp", axis=2, tiled=True)
    gate_pre = jnp.einsum(
        "esd,edf->esf", column_piece, routed_gate_weight, preferred_element_type=F32
    )
    up_pre = jnp.einsum("esd,edf->esf", column_piece, routed_up_weight, preferred_element_type=F32)
    hidden = (jax.nn.silu(gate_pre) * up_pre).astype(BF16)
    shared_hidden = (
        jax.nn.silu(jnp.dot(normed, shared_gate_weight, preferred_element_type=F32))
        * jnp.dot(normed, shared_up_weight, preferred_element_type=F32)
    ).astype(BF16)
    whole_mix, whole_hidden, whole_shared = one_gather(
        (mixer_normed, hidden, shared_hidden), "tp", (1, 2, 1)
    )
    mixer_output = jnp.dot(whole_mix, mixer_output_weight, preferred_element_type=F32).astype(BF16)
    expert_result = jnp.einsum(
        "esf,efd->esd", whole_hidden, routed_down_weight, preferred_element_type=F32
    ).astype(BF16)
    returned = lax.all_to_all(expert_result, "ep", split_axis=1, concat_axis=0, tiled=True)
    returned = returned.reshape(experts * capacity, col_width)
    weight_high = high(weight)
    contract = (((0,), (0,)), ((), ()))
    routed_sum = jnp.zeros((rows_local, col_width), F32)
    for part in (weight_high, weight - weight_high):
        spread_part = jnp.where(taken, part[:, None, :], 0.0).astype(BF16)
        spread_part = spread_part.reshape(experts * capacity, rows_local)
        routed_sum = routed_sum + lax.dot_general(
            spread_part, returned, contract, preferred_element_type=F32
        )
    shared_result = jnp.dot(whole_shared, shared_down_weight, preferred_element_type=F32)
    routed_out = (routed_sum + shared_result).astype(BF16)
    return (mixer_output, routed_out)


def solution(mesh):
    return jax.shard_map(
        on_device,
        mesh=mesh,
        in_specs=(
            P("ep", "tp"),
            P("ep", "tp"),
            P("ep", "tp"),
            P("ep", "tp"),
            P("ep", "tp"),
            P("ep", "tp"),
            P("tp"),
            P("tp"),
            P(None, "tp"),
            P(None, "tp"),
            P(None, "tp"),
            P("tp"),
            P(None, "tp"),
            P("ep", None),
            P(),
            P("ep", None),
            P("ep", None),
            P("ep", None, "tp"),
            P("ep", None, "tp"),
            P("ep", None, "tp"),
            P(None, "tp"),
            P(None, "tp"),
            P(None, "tp"),
        ),
        out_specs=(P("ep", "tp"), P("ep", "tp")),
        check_vma=False,
    )
```

```python
import jax
import jax.numpy as jnp
from jax import lax
from jax.experimental import pallas as pl
from jax.experimental.layout import Layout, with_layout_constraint
from jax.experimental.pallas import tpu as pltpu
from jax.sharding import PartitionSpec as P

HEAD_DIM = 64
STATE = 128
CONV_TAPS = 4
BLOCK = 128
TOP_K = 4
epsilon = 1e-05
F32 = jnp.float32
BF16 = jnp.bfloat16


def passed_along(x, axis, by):
    size = lax.axis_size(axis)
    pairs = [(i, i + by) for i in range(size) if 0 <= i + by < size]
    return lax.ppermute(x, axis, pairs)


def high(x):
    return lax.reduce_precision(x, 8, 7)


def three_parts(x):
    a = high(x)
    b = high(x - a)
    return a, b, x - a - b


def conv_silu(tail_rows, source, weights):
    length = source.shape[0]
    padded = jnp.concatenate([tail_rows, source], axis=0)
    total_sum = jnp.zeros(source.shape, F32)
    for tap_index in range(CONV_TAPS):
        total_sum = (
            total_sum
            + padded[tap_index : tap_index + length].astype(F32) * weights[tap_index]
        )
    return jax.nn.silu(total_sum).astype(BF16)


def state_before(log_total, total_state):
    heads = log_total.shape[0]
    count = lax.axis_size("ep")
    place = lax.axis_index("ep")
    parts = jnp.stack(three_parts(log_total)).reshape(1, 3 * heads)
    row = jnp.pad(parts, ((0, 15), (0, STATE - 3 * heads)))
    rows = heads * HEAD_DIM
    payload = jnp.concatenate([total_state.reshape(rows, STATE), row], axis=0).astype(BF16)
    gathered = lax.all_gather(payload, "ep")
    tail = gathered[:, rows, : 3 * heads].astype(F32).reshape(count, 3, heads)
    logs = jnp.sum(tail, axis=1)
    at = jnp.arange(count)
    between = (at[None, :] > at[:, None]) & (at[None, :] < place)
    spans = jnp.sum(jnp.where(between[:, :, None], logs[None], 0.0), axis=1)
    weights = jnp.where((at < place)[:, None], jnp.exp(spans), 0.0)
    wide = jnp.repeat(weights, HEAD_DIM, axis=1)[:, :, None]
    summed = jnp.sum(gathered[:, :rows, :].astype(F32) * wide, axis=0)
    return summed.reshape(heads, HEAD_DIM, STATE)


SIDE = 4
HALF = 12
PADDED = 16
ROW_GROUPS = [[SIDE * y + x for x in range(SIDE)] for y in range(SIDE)]
COLUMN_GROUPS = [[SIDE * y + x for y in range(SIDE)] for x in range(SIDE)]


def along(x, groups):
    return lax.all_to_all(
        x, "tp", split_axis=0, concat_axis=0, tiled=True, axis_index_groups=groups
    )


def shown_to_row(x):
    return along(jnp.broadcast_to(x[None], (SIDE,) + x.shape), ROW_GROUPS)


def places(index_t, weight_t, experts):
    rows = index_t.shape[1]
    ids = jnp.arange(experts, dtype=jnp.int32)[:, None]
    named = jnp.zeros((experts, rows), F32)
    weight = jnp.zeros((experts, rows), F32)
    for k in range(TOP_K):
        hit = index_t[k][None, :] == ids
        named = jnp.where(hit, 1.0, named)
        weight = jnp.where(hit, weight_t[k][None, :], weight)
    at = jnp.arange(rows)
    earlier = (at[:, None] < at[None, :]).astype(BF16)
    place = jnp.dot(named.astype(BF16), earlier, preferred_element_type=F32)
    return jnp.where(named > 0.0, place, -1.0), weight


def slot_numbers(half):
    i = jnp.arange(PADDED, dtype=jnp.int32)
    return jnp.where(i < HALF, half * HALF + i, -7).astype(F32)


def pre_kernel(x_ref, g_ref, u_ref, h_ref):
    k = x_ref.shape[2]
    dims = (((1,), (1,)), ((), ()))
    gate = jnp.zeros(h_ref.shape, F32)
    up = jnp.zeros(h_ref.shape, F32)
    for n in range(SIDE):
        x = x_ref[n]
        g = g_ref[:, n * k : (n + 1) * k]
        u = u_ref[:, n * k : (n + 1) * k]
        gate = gate + lax.dot_general(x, g, dims, preferred_element_type=F32)
        up = up + lax.dot_general(x, u, dims, preferred_element_type=F32)
    h_ref[...] = (gate / (1.0 + jnp.exp(-gate)) * up).astype(BF16)


def expert_hidden(x, g, u):
    slots = x.shape[1]
    ff, width = g.shape
    step = 128
    return pl.pallas_call(
        pre_kernel,
        grid=(slots // step,),
        in_specs=[
            pl.BlockSpec((SIDE, step, x.shape[2]), lambda i: (0, i, 0)),
            pl.BlockSpec((ff, width), lambda i: (0, 0)),
            pl.BlockSpec((ff, width), lambda i: (0, 0)),
        ],
        out_specs=pl.BlockSpec((step, ff), lambda i: (i, 0)),
        out_shape=jax.ShapeDtypeStruct((slots, ff), BF16),
        cost_estimate=pl.CostEstimate(
            flops=4 * slots * ff * width, bytes_accessed=4 * 2**20, transcendentals=slots * ff
        ),
    )(x, g, u)


def down_kernel(h_ref, w_ref, o_ref):
    k = h_ref.shape[2]
    for m in range(SIDE):
        total = jnp.zeros(o_ref.shape[1:], F32)
        for n in range(SIDE):
            w = w_ref[m, n * k : (n + 1) * k, :]
            total = total + jnp.dot(h_ref[n], w, preferred_element_type=F32)
        o_ref[m] = total.astype(BF16)


def expert_down(h, w):
    slots = h.shape[1]
    width, columns = w.shape[1:]
    step = 128
    return pl.pallas_call(
        down_kernel,
        grid=(slots // step,),
        in_specs=[
            pl.BlockSpec((SIDE, step, h.shape[2]), lambda i: (0, i, 0)),
            pl.BlockSpec(w.shape, lambda i: (0, 0, 0)),
        ],
        out_specs=pl.BlockSpec((SIDE, step, columns), lambda i: (0, i, 0)),
        out_shape=jax.ShapeDtypeStruct((SIDE, slots, columns), BF16),
        cost_estimate=pl.CostEstimate(
            flops=2 * SIDE * slots * width * columns, bytes_accessed=3 * 2**20, transcendentals=0
        ),
    )(h, w)


def last_kernel(g_ref, w_ref, s_ref, m_ref, r_ref, m_acc, r_acc):
    n, _, lanes = g_ref.shape
    rows = m_ref.shape[0]

    @pl.when(pl.program_id(0) == 0)
    def _():
        m_acc[...] = jnp.zeros_like(m_acc)
        r_acc[...] = jnp.zeros_like(r_acc)

    mix = m_acc[...]
    shared = r_acc[...]
    half = lanes // 2
    for t in range(n):
        for c in range(2):
            at = (2 * t + c) * lanes
            piece = g_ref[t, c * rows : (c + 1) * rows, :]
            mix = mix + jnp.dot(piece, w_ref[at : at + lanes, :], preferred_element_type=F32)
        pair = g_ref[t, 2 * rows :, :]
        w = s_ref[t * half : (t + 1) * half, :]
        parts = [
            jnp.dot(pair[:, c * half : (c + 1) * half], w, preferred_element_type=F32)
            for c in range(2)
        ]
        shared = shared + jnp.concatenate(parts, axis=0)
    m_acc[...] = mix
    r_acc[...] = shared

    @pl.when(pl.program_id(0) == pl.num_programs(0) - 1)
    def _():
        m_ref[...] = mix.astype(BF16)
        r_ref[...] = shared


def last_products(gathered, mix_weight, shared_weight, rows):
    count, tall, lanes = gathered.shape
    columns = mix_weight.shape[1]
    n = 4
    return pl.pallas_call(
        last_kernel,
        grid=(count // n,),
        in_specs=[
            pl.BlockSpec((n, tall, lanes), lambda i: (i, 0, 0)),
            pl.BlockSpec((n * 2 * lanes, columns), lambda i: (i, 0)),
            pl.BlockSpec((n * lanes // 2, columns), lambda i: (i, 0)),
        ],
        out_specs=[
            pl.BlockSpec((rows, columns), lambda i: (0, 0)),
            pl.BlockSpec((rows, columns), lambda i: (0, 0)),
        ],
        out_shape=[
            jax.ShapeDtypeStruct((rows, columns), BF16),
            jax.ShapeDtypeStruct((rows, columns), F32),
        ],
        scratch_shapes=[pltpu.VMEM((rows, columns), F32), pltpu.VMEM((rows, columns), F32)],
        cost_estimate=pl.CostEstimate(
            flops=2 * rows * columns * (mix_weight.shape[0] + shared_weight.shape[0]),
            bytes_accessed=4 * 2**20,
            transcendentals=0,
        ),
    )(gathered, mix_weight, shared_weight)


def on_device(
    mixer_value_input,
    input_state_matrix,
    output_state_matrix,
    output_gate_input,
    step_input,
    extra_log_decay,
    head_log_decay,
    head_skip_scale,
    value_kernel,
    input_matrix_kernel,
    output_matrix_kernel,
    mixer_norm_scale,
    mixer_output_weight,
    second_token_rows,
    expert_norm_scale,
    routed_expert_index,
    routed_expert_weight,
    routed_gate_weight,
    routed_up_weight,
    routed_down_weight,
    shared_gate_weight,
    shared_up_weight,
    shared_down_weight,
):
    length = mixer_value_input.shape[0]
    heads_local = step_input.shape[1]
    width_x = mixer_value_input.shape[1]
    width_b = input_state_matrix.shape[1]
    groups_local = width_b // STATE
    head_ratio = heads_local // groups_local
    nblocks = length // BLOCK
    lead_row = length - CONV_TAPS + 1
    edge_rows = jnp.concatenate(
        [
            mixer_value_input[lead_row:],
            input_state_matrix[lead_row:],
            output_state_matrix[lead_row:],
        ],
        axis=1,
    )
    tail_rows = passed_along(edge_rows, "ep", 1)
    values = conv_silu(tail_rows[:, :width_x], mixer_value_input, value_kernel)
    in_mat = conv_silu(
        tail_rows[:, width_x : width_x + width_b], input_state_matrix, input_matrix_kernel
    )
    out_mat = conv_silu(
        tail_rows[:, width_x + width_b :], output_state_matrix, output_matrix_kernel
    )
    step_length = jax.nn.softplus(step_input)
    decay_logarithm = -jnp.exp(head_log_decay)[None, :] * step_length + extra_log_decay
    running = jnp.cumsum(decay_logarithm.reshape(nblocks, BLOCK, heads_local), axis=1)
    value_wide = values.astype(F32).reshape(nblocks, BLOCK, heads_local, HEAD_DIM)
    scaled = value_wide * step_length.reshape(nblocks, BLOCK, heads_local)[..., None]
    in_blocks = in_mat.reshape(nblocks, BLOCK, groups_local, STATE)
    out_blocks = out_mat.reshape(nblocks, BLOCK, groups_local, STATE)
    scores = jnp.einsum("bign,bjgn->bgij", out_blocks, in_blocks, preferred_element_type=F32)
    scores = jnp.repeat(scores, head_ratio, axis=1)
    spread = jnp.transpose(running[:, :, None, :] - running[:, None, :, :], (0, 3, 1, 2))
    lower_mask = jnp.tril(jnp.ones((BLOCK, BLOCK), bool))[None, None]
    decay_mat = jnp.where(lower_mask, jnp.exp(jnp.where(lower_mask, spread, 0.0)), 0.0)
    inside = jnp.einsum("bhij,bjhp->bihp", scores * decay_mat, scaled)
    out_head = jnp.repeat(out_blocks.astype(F32), head_ratio, axis=2)
    in_head = jnp.repeat(in_blocks.astype(F32), head_ratio, axis=2)
    block_logs = running[:, -1]
    to_end = jnp.exp(block_logs[:, None, :] - running)
    block_state = jnp.einsum("bjhn,bjh,bjhp->bhpn", in_head, to_end, scaled)
    carried = jnp.zeros((heads_local, HEAD_DIM, STATE), F32)
    before = []
    for b in range(nblocks):
        before.append(carried)
        carried = carried * jnp.exp(block_logs[b])[:, None, None] + block_state[b]
    local_prev = jnp.stack(before)
    before_logs = jnp.cumsum(block_logs, axis=0) - block_logs
    incoming = state_before(jnp.sum(block_logs, axis=0), carried)
    entering = local_prev + jnp.exp(before_logs)[:, :, None, None] * incoming[None]
    carried_term = jnp.einsum("bihn,bhpn->bihp", out_head, entering) * jnp.exp(running)[..., None]
    mixed_heads = (inside + carried_term).reshape(length, heads_local, HEAD_DIM)
    mixed_heads = mixed_heads + head_skip_scale[None, :, None] * value_wide.reshape(
        length, heads_local, HEAD_DIM
    )
    gated_heads = mixed_heads * jax.nn.silu(output_gate_input.astype(F32)).reshape(
        length, heads_local, HEAD_DIM
    )
    grouped = gated_heads.reshape(length, groups_local, head_ratio * HEAD_DIM)
    grouped = grouped * lax.rsqrt(jnp.mean(grouped * grouped, axis=-1, keepdims=True) + epsilon)
    mixer_normed = (grouped.reshape(length, width_x) * mixer_norm_scale).astype(BF16)

    rows_local = second_token_rows.shape[0]
    model_width = second_token_rows.shape[1]
    local_experts = routed_gate_weight.shape[0]
    ep_count = lax.axis_size("ep")
    experts = local_experts * ep_count
    tp_place = lax.axis_index("tp")
    down, across = tp_place // SIDE, tp_place % SIDE
    my_expert, my_half = down // 2, down % 2
    columns = routed_down_weight.shape[2]
    part_ff = routed_gate_weight.shape[2]
    share = model_width // SIDE

    gate_up = jnp.stack(
        [jnp.swapaxes(routed_gate_weight, 1, 2), jnp.swapaxes(routed_up_weight, 1, 2)]
    )
    gate_up = jnp.concatenate([gate_up[0], gate_up[1]], axis=1)
    gate_up = jnp.stack([gate_up[0], gate_up[0], gate_up[1], gate_up[1]])
    gate_up = along(gate_up, COLUMN_GROUPS)
    gate_w = gate_up[:, :part_ff].reshape(SIDE * part_ff, model_width)
    up_w = gate_up[:, part_ff:].reshape(SIDE * part_ff, model_width)
    down_w = routed_down_weight.reshape(local_experts, SIDE, SIDE, part_ff, columns)
    down_w = jnp.swapaxes(down_w, 1, 2).reshape(routed_down_weight.shape)
    down_w = along(jnp.stack([down_w[0], down_w[0], down_w[1], down_w[1]]), COLUMN_GROUPS)

    rows_wide = second_token_rows.astype(F32)
    normed = (
        rows_wide
        * lax.rsqrt(jnp.mean(rows_wide * rows_wide, axis=-1, keepdims=True) + epsilon)
        * expert_norm_scale
    ).astype(BF16)
    place, weight = places(routed_expert_index.T, routed_expert_weight.T, experts)
    by_owner = place.reshape(ep_count, local_experts, rows_local)
    mine = lax.dynamic_index_in_dim(by_owner, my_expert, 1, False)
    taken = mine[:, None, :] == slot_numbers(my_half)[None, :, None]
    one_hot = taken.astype(BF16).reshape(ep_count * PADDED, rows_local)
    my_share = lax.dynamic_slice_in_dim(normed, across * share, share, 1)
    outgoing = jnp.dot(one_hot, my_share, preferred_element_type=F32).astype(BF16)
    arrived = lax.all_to_all(
        outgoing.reshape(ep_count, PADDED, share), "ep", split_axis=0, concat_axis=0, tiled=True
    )
    arrived = shown_to_row(arrived.reshape(ep_count * PADDED, share))
    hidden = shown_to_row(expert_hidden(arrived, gate_w, up_w))
    result = along(expert_down(hidden, down_w), COLUMN_GROUPS)
    result = jnp.swapaxes(result.reshape(SIDE, ep_count, PADDED, columns), 0, 1)
    result = result.reshape(ep_count, SIDE * PADDED, columns)
    returned = lax.all_to_all(result, "ep", split_axis=0, concat_axis=0, tiled=True)
    returned = returned.reshape(ep_count * SIDE * PADDED, columns)

    shared_hidden = (
        jax.nn.silu(jnp.dot(normed, shared_gate_weight, preferred_element_type=F32))
        * jnp.dot(normed, shared_up_weight, preferred_element_type=F32)
    ).astype(BF16)
    half_rows = rows_local // 2
    lanes = width_x // 2
    payload = jnp.concatenate(
        [
            mixer_normed[:, :lanes],
            mixer_normed[:, lanes:],
            jnp.concatenate([shared_hidden[:half_rows], shared_hidden[half_rows:]], axis=1),
        ],
        axis=0,
    )
    payload = with_layout_constraint(payload, Layout(major_to_minor=(0, 1)))
    gathered = lax.all_gather(payload, "tp")
    mixer_output, shared_result = last_products(
        gathered, mixer_output_weight, shared_down_weight, rows_local
    )

    halves = jnp.stack([slot_numbers(0), slot_numbers(1)])
    taken = by_owner[:, :, None, None, :] == halves[None, None, :, :, None]
    weight = weight.reshape(ep_count, local_experts, 1, 1, rows_local)
    weight_high = high(weight)
    contract = (((0,), (0,)), ((), ()))
    routed_sum = shared_result
    for part in (weight_high, weight - weight_high):
        spread_part = jnp.where(taken, part, 0.0).astype(BF16).reshape(-1, rows_local)
        routed_sum = routed_sum + lax.dot_general(
            spread_part, returned, contract, preferred_element_type=F32
        )
    routed_out = routed_sum.astype(BF16)
    return (mixer_output, routed_out)


def solution(mesh):
    return jax.shard_map(
        on_device,
        mesh=mesh,
        in_specs=(
            P("ep", "tp"),
            P("ep", "tp"),
            P("ep", "tp"),
            P("ep", "tp"),
            P("ep", "tp"),
            P("ep", "tp"),
            P("tp"),
            P("tp"),
            P(None, "tp"),
            P(None, "tp"),
            P(None, "tp"),
            P("tp"),
            P(None, "tp"),
            P("ep", None),
            P(),
            P("ep", None),
            P("ep", None),
            P("ep", None, "tp"),
            P("ep", None, "tp"),
            P("ep", None, "tp"),
            P(None, "tp"),
            P(None, "tp"),
            P(None, "tp"),
        ),
        out_specs=(P("ep", "tp"), P("ep", "tp")),
        check_vma=False,
    )
```

```python
import jax
import jax.numpy as jnp
from jax import lax
from jax.experimental import pallas as pl
from jax.experimental.pallas import tpu as pltpu
from jax.sharding import PartitionSpec as P

HEAD_DIM = 64
STATE = 128
CONV_TAPS = 4
BLOCK = 128
TOP_K = 4
epsilon = 1e-05
F32 = jnp.float32
BF16 = jnp.bfloat16


def whole(shape):
    return pl.BlockSpec(shape, lambda *_: (0,) * len(shape))


SCALAR = pl.BlockSpec(memory_space=pltpu.SMEM)


def passed_along(x, axis, by):
    size = lax.axis_size(axis)
    pairs = [(i, i + by) for i in range(size) if 0 <= i + by < size]
    return lax.ppermute(x, axis, pairs)


def high(x):
    return lax.reduce_precision(x, 8, 7)


def three_parts(x):
    a = high(x)
    b = high(x - a)
    return a, b, x - a - b


def conv_silu(tail_rows, source, weights):
    length = source.shape[0]
    padded = jnp.concatenate([tail_rows, source], axis=0)
    total_sum = jnp.zeros(source.shape, F32)
    for tap_index in range(CONV_TAPS):
        total_sum = (
            total_sum
            + padded[tap_index : tap_index + length].astype(F32) * weights[tap_index]
        )
    return jax.nn.silu(total_sum).astype(BF16)


def states_gathered(log_total, total_state):
    heads = log_total.shape[0]
    parts = jnp.stack(three_parts(log_total)).reshape(1, 3 * heads)
    row = jnp.pad(parts, ((0, 15), (0, STATE - 3 * heads)))
    payload = jnp.concatenate([total_state.reshape(heads * HEAD_DIM, STATE), row], axis=0)
    return lax.all_gather(payload.astype(BF16), "ep")


def late_kernel(
    at_ref,
    g_ref,
    v_ref,
    b_ref,
    c_ref,
    cum_ref,
    cum_t_ref,
    step_t_ref,
    gate_ref,
    skip_ref,
    norm_ref,
    first_ref,
    shared_ref,
    out_ref,
    mixed_ref,
):
    place = at_ref[0]
    count = g_ref.shape[0]
    heads = cum_ref.shape[1]
    rows, width = v_ref.shape
    top = heads * HEAD_DIM
    tail = g_ref[:, top, :]
    row = lax.broadcasted_iota(jnp.int32, (count, count), 0)
    col = lax.broadcasted_iota(jnp.int32, (count, count), 1)
    between = jnp.where((col > row) & (col < place), 1.0, 0.0).astype(BF16)
    parts = jnp.dot(between, tail, preferred_element_type=F32)
    spans = parts[:, :heads] + parts[:, heads : 2 * heads] + parts[:, 2 * heads : 3 * heads]
    device = lax.broadcasted_iota(jnp.int32, (count, heads), 0)
    weights = jnp.where(device < place, jnp.exp(spans), 0.0)
    pieces = []
    for h in range(heads):
        total = jnp.zeros((HEAD_DIM, STATE), F32)
        for j in range(count):
            state = g_ref[j, h * HEAD_DIM : (h + 1) * HEAD_DIM, :].astype(F32)
            total = total + state * weights[j : j + 1, h : h + 1]
        pieces.append(total)
    contract = (((1,), (1,)), ((), ()))
    i = lax.broadcasted_iota(jnp.int32, (BLOCK, BLOCK), 0)
    j = lax.broadcasted_iota(jnp.int32, (BLOCK, BLOCK), 1)
    lower = i >= j
    for block in range(rows // BLOCK):
        at = slice(block * BLOCK, (block + 1) * BLOCK)
        c = c_ref[at, :]
        scores = lax.dot_general(c, b_ref[at, :], contract, preferred_element_type=F32)
        for h in range(heads):
            lanes = slice(h * HEAD_DIM, (h + 1) * HEAD_DIM)
            cum = cum_ref[at, h : h + 1]
            spread = cum - cum_t_ref[h : h + 1, at]
            decay = jnp.where(lower, jnp.exp(jnp.where(lower, spread, 0.0)), 0.0)
            inner = (scores * decay * step_t_ref[h : h + 1, at]).astype(BF16)
            inside = jnp.dot(inner, v_ref[at, lanes], preferred_element_type=F32)
            state = pieces[h].astype(BF16)
            carried = lax.dot_general(c, state, contract, preferred_element_type=F32)
            mixed_ref[at, lanes] = inside + carried * jnp.exp(cum)
            if block + 1 < rows // BLOCK:
                last = jnp.exp(cum_ref[(block + 1) * BLOCK - 1 : (block + 1) * BLOCK, h : h + 1])
                pieces[h] = pieces[h] * last + first_ref[lanes, :]
    gate = gate_ref[...].astype(F32)
    mixed = mixed_ref[...] + skip_ref[...] * v_ref[...].astype(F32)
    mixed = mixed * (gate / (1.0 + jnp.exp(-gate)))
    mean = jnp.mean(mixed * mixed, axis=-1, keepdims=True)
    normed = (mixed * lax.rsqrt(mean + epsilon) * norm_ref[...]).astype(BF16)
    half = width // 2
    out_ref[:rows, :] = normed[:, :half]
    out_ref[rows : 2 * rows, :] = normed[:, half:]
    out_ref[2 * rows :, :] = jnp.concatenate(
        [shared_ref[: rows // 2, :], shared_ref[rows // 2 :, :]], axis=1
    )


def late_mixer(place, gathered, v, b, c, cum, cum_t, step_t, gate, skip, norm, first, shared):
    rows, width = v.shape
    operands = (gathered, v, b, c, cum, cum_t, step_t, gate, skip, norm, first, shared)
    return pl.pallas_call(
        late_kernel,
        grid=(1,),
        in_specs=[SCALAR] + [whole(o.shape) for o in operands],
        out_specs=whole((2 * rows + rows // 2, width // 2)),
        out_shape=jax.ShapeDtypeStruct((2 * rows + rows // 2, width // 2), BF16),
        scratch_shapes=[pltpu.VMEM((rows, width), F32)],
        cost_estimate=pl.CostEstimate(
            flops=2**28, bytes_accessed=4 * 2**20, transcendentals=2**18
        ),
    )(place, *operands)


SIDE = 4
HALF = 12
PADDED = 16
ROW_GROUPS = [[SIDE * y + x for x in range(SIDE)] for y in range(SIDE)]
COLUMN_GROUPS = [[SIDE * y + x for y in range(SIDE)] for x in range(SIDE)]


def along(x, groups):
    return lax.all_to_all(
        x, "tp", split_axis=0, concat_axis=0, tiled=True, axis_index_groups=groups
    )


def shown_to_row(x):
    return along(jnp.broadcast_to(x[None], (SIDE,) + x.shape), ROW_GROUPS)


def places(index_t, weight_t, experts):
    rows = index_t.shape[1]
    ids = jnp.arange(experts, dtype=jnp.int32)[:, None]
    named = jnp.zeros((experts, rows), F32)
    weight = jnp.zeros((experts, rows), F32)
    for k in range(TOP_K):
        hit = index_t[k][None, :] == ids
        named = jnp.where(hit, 1.0, named)
        weight = jnp.where(hit, weight_t[k][None, :], weight)
    at = jnp.arange(rows)
    earlier = (at[:, None] < at[None, :]).astype(BF16)
    place = jnp.dot(named.astype(BF16), earlier, preferred_element_type=F32)
    return jnp.where(named > 0.0, place, -1.0), weight


def slot_numbers(half):
    i = jnp.arange(PADDED, dtype=jnp.int32)
    return jnp.where(i < HALF, half * HALF + i, -7).astype(F32)


def dispatch_kernel(at_ref, index_ref, rows_ref, gain_ref, out_ref, normed_ref):
    y, x = at_ref[0] // SIDE, at_ref[0] % SIDE
    wide = rows_ref[...].astype(F32)
    mean = jnp.mean(wide * wide, axis=-1, keepdims=True)
    normed_ref[...] = (wide * lax.rsqrt(mean + epsilon) * gain_ref[...]).astype(BF16)
    slots, share = out_ref.shape
    rows = rows_ref.shape[0]
    line = lax.broadcasted_iota(jnp.int32, (slots, rows), 0)
    expert = (line // PADDED) * 2 + y // 2
    inner = line % PADDED
    slot = jnp.where(inner < HALF, inner + (y % 2) * HALF, -7)
    named = index_ref[0:1, :] == expert
    for k in range(1, TOP_K):
        named = named | (index_ref[k : k + 1, :] == expert)
    before = lax.broadcasted_iota(jnp.int32, (rows, rows), 0)
    after = lax.broadcasted_iota(jnp.int32, (rows, rows), 1)
    earlier = jnp.where(before < after, 1.0, 0.0).astype(BF16)
    ones = jnp.where(named, 1.0, 0.0).astype(BF16)
    place = jnp.dot(ones, earlier, preferred_element_type=F32)
    taken = named & (place == slot.astype(F32))
    one_hot = jnp.where(taken, 1.0, 0.0).astype(BF16)
    mine = normed_ref[:, pl.ds(pl.multiple_of(x * share, share), share)]
    out_ref[...] = jnp.dot(one_hot, mine, preferred_element_type=F32).astype(BF16)


def dispatch(at, index_t, rows, gain, owners):
    count, width = rows.shape
    return pl.pallas_call(
        dispatch_kernel,
        in_specs=[SCALAR, whole(index_t.shape), whole(rows.shape), whole((1, width))],
        out_specs=[whole((owners * PADDED, width // SIDE)), whole((count, width))],
        out_shape=[
            jax.ShapeDtypeStruct((owners * PADDED, width // SIDE), BF16),
            jax.ShapeDtypeStruct((count, width), BF16),
        ],
        grid=(1,),
        cost_estimate=pl.CostEstimate(
            flops=2 * owners * PADDED * count * width // SIDE,
            bytes_accessed=3 * 2**20,
            transcendentals=0,
        ),
    )(at, index_t, rows, gain.reshape(1, width))


def sources(y):
    return [y, (y + SIDE - 1) % SIDE, (y + 1) % SIDE, (y + 2) % SIDE]


def pre_kernel(x_ref, w0_ref, w1_ref, w2_ref, w3_ref, h_ref, g_ref, u_ref):
    k = x_ref.shape[2]
    ff = w0_ref.shape[0] // 2

    @pl.when(pl.program_id(0) == 0)
    def _():
        for j, w_ref in enumerate((w0_ref, w1_ref, w2_ref, w3_ref)):
            g_ref[j * ff : (j + 1) * ff, :] = w_ref[:ff, :]
            u_ref[j * ff : (j + 1) * ff, :] = w_ref[ff:, :]

    dims = (((1,), (1,)), ((), ()))
    gate = jnp.zeros(h_ref.shape, F32)
    up = jnp.zeros(h_ref.shape, F32)
    for n in range(SIDE):
        x = x_ref[n]
        g = g_ref[:, n * k : (n + 1) * k]
        u = u_ref[:, n * k : (n + 1) * k]
        gate = gate + lax.dot_general(x, g, dims, preferred_element_type=F32)
        up = up + lax.dot_general(x, u, dims, preferred_element_type=F32)
    h_ref[...] = (gate / (1.0 + jnp.exp(-gate)) * up).astype(BF16)


def expert_hidden(x, weights):
    slots = x.shape[1]
    ff, width = weights[0].shape[0] // 3, weights[0].shape[1]
    step = 256
    return pl.pallas_call(
        pre_kernel,
        grid=(slots // step,),
        in_specs=[pl.BlockSpec((SIDE, step, x.shape[2]), lambda i: (0, i, 0))]
        + [whole((2 * ff, width))] * SIDE,
        out_specs=pl.BlockSpec((step, SIDE * ff), lambda i: (i, 0)),
        out_shape=jax.ShapeDtypeStruct((slots, SIDE * ff), BF16),
        scratch_shapes=[pltpu.VMEM((SIDE * ff, width), BF16)] * 2,
        cost_estimate=pl.CostEstimate(
            flops=4 * slots * SIDE * ff * width,
            bytes_accessed=4 * 2**20,
            transcendentals=slots * SIDE * ff,
        ),
    )(x, *weights)


def down_kernel(at_ref, h_ref, w0_ref, w1_ref, w2_ref, w3_ref, o_ref):
    y = at_ref[0] // SIDE
    order = sources(y)
    columns = o_ref.shape[2]
    for owner, w_ref in zip(order, (w0_ref, w1_ref, w2_ref, w3_ref)):
        total = jnp.zeros(o_ref.shape[1:], F32)
        for n in range(SIDE):
            blocks = [
                w_ref[:, pl.ds(pl.multiple_of((j * SIDE + n) * columns, columns), columns)]
                for j in order
            ]
            w = jnp.concatenate(blocks, axis=0)
            total = total + jnp.dot(h_ref[n], w, preferred_element_type=F32)
        o_ref[owner] = total.astype(BF16)


def expert_down(at, h, weights):
    slots = h.shape[1]
    ff, width = weights[0].shape[0] // 3, weights[0].shape[1]
    columns = width // (SIDE * SIDE)
    step = 256
    return pl.pallas_call(
        down_kernel,
        grid=(slots // step,),
        in_specs=[SCALAR, pl.BlockSpec((SIDE, step, h.shape[2]), lambda i: (0, i, 0))]
        + [pl.BlockSpec((ff, width), lambda i: (2, 0))] * SIDE,
        out_specs=pl.BlockSpec((SIDE, step, columns), lambda i: (0, i, 0)),
        out_shape=jax.ShapeDtypeStruct((SIDE, slots, columns), BF16),
        cost_estimate=pl.CostEstimate(
            flops=2 * SIDE * slots * SIDE * SIDE * ff * columns,
            bytes_accessed=3 * 2**20,
            transcendentals=0,
        ),
    )(at, h, *weights)


def shifted_down(x, by):
    pairs = [
        (SIDE * y + c, SIDE * ((y + by) % SIDE) + c) for y in range(SIDE) for c in range(SIDE)
    ]
    return lax.ppermute(x, "tp", pairs)


def last_kernel(g_ref, w_ref, s_ref, m_ref, r_ref, m_acc, r_acc):
    n, _, lanes = g_ref.shape
    rows = m_ref.shape[0]

    @pl.when(pl.program_id(0) == 0)
    def _():
        m_acc[...] = jnp.zeros_like(m_acc)
        r_acc[...] = jnp.zeros_like(r_acc)

    mix = m_acc[...]
    shared = r_acc[...]
    half = lanes // 2
    for t in range(n):
        for c in range(2):
            at = (2 * t + c) * lanes
            piece = g_ref[t, c * rows : (c + 1) * rows, :]
            mix = mix + jnp.dot(piece, w_ref[at : at + lanes, :], preferred_element_type=F32)
        pair = g_ref[t, 2 * rows :, :]
        w = s_ref[t * half : (t + 1) * half, :]
        parts = [
            jnp.dot(pair[:, c * half : (c + 1) * half], w, preferred_element_type=F32)
            for c in range(2)
        ]
        shared = shared + jnp.concatenate(parts, axis=0)
    m_acc[...] = mix
    r_acc[...] = shared

    @pl.when(pl.program_id(0) == pl.num_programs(0) - 1)
    def _():
        m_ref[...] = mix.astype(BF16)
        r_ref[...] = shared


def last_products(gathered, mix_weight, shared_weight, rows):
    count, tall, lanes = gathered.shape
    columns = mix_weight.shape[1]
    n = 4
    return pl.pallas_call(
        last_kernel,
        grid=(count // n,),
        in_specs=[
            pl.BlockSpec((n, tall, lanes), lambda i: (i, 0, 0)),
            pl.BlockSpec((n * 2 * lanes, columns), lambda i: (i, 0)),
            pl.BlockSpec((n * lanes // 2, columns), lambda i: (i, 0)),
        ],
        out_specs=[
            pl.BlockSpec((rows, columns), lambda i: (0, 0)),
            pl.BlockSpec((rows, columns), lambda i: (0, 0)),
        ],
        out_shape=[
            jax.ShapeDtypeStruct((rows, columns), BF16),
            jax.ShapeDtypeStruct((rows, columns), F32),
        ],
        scratch_shapes=[pltpu.VMEM((rows, columns), F32), pltpu.VMEM((rows, columns), F32)],
        cost_estimate=pl.CostEstimate(
            flops=2 * rows * columns * (mix_weight.shape[0] + shared_weight.shape[0]),
            bytes_accessed=4 * 2**20,
            transcendentals=0,
        ),
    )(gathered, mix_weight, shared_weight)


def step(
    mixer_value_input,
    input_state_matrix,
    output_state_matrix,
    output_gate_input,
    step_input,
    extra_log_decay,
    head_log_decay,
    head_skip_scale,
    value_kernel,
    input_matrix_kernel,
    output_matrix_kernel,
    mixer_norm_scale,
    mixer_output_weight,
    second_token_rows,
    expert_norm_scale,
    routed_expert_index,
    routed_expert_weight,
    routed_gate_weight,
    routed_up_weight,
    routed_down_weight,
    shared_gate_weight,
    shared_up_weight,
    shared_down_weight,
):
    length = mixer_value_input.shape[0]
    heads_local = step_input.shape[1]
    width_x = mixer_value_input.shape[1]
    width_b = input_state_matrix.shape[1]
    groups_local = width_b // STATE
    head_ratio = heads_local // groups_local
    nblocks = length // BLOCK
    lead_row = length - CONV_TAPS + 1
    edge_rows = jnp.concatenate(
        [
            mixer_value_input[lead_row:],
            input_state_matrix[lead_row:],
            output_state_matrix[lead_row:],
        ],
        axis=1,
    )
    tail_rows = passed_along(edge_rows, "ep", 1)
    values = conv_silu(tail_rows[:, :width_x], mixer_value_input, value_kernel)
    in_mat = conv_silu(
        tail_rows[:, width_x : width_x + width_b], input_state_matrix, input_matrix_kernel
    )
    out_mat = conv_silu(
        tail_rows[:, width_x + width_b :], output_state_matrix, output_matrix_kernel
    )
    step_length = jax.nn.softplus(step_input)
    decay_logarithm = -jnp.exp(head_log_decay)[None, :] * step_length + extra_log_decay
    running = jnp.cumsum(decay_logarithm.reshape(nblocks, BLOCK, heads_local), axis=1)
    value_wide = values.astype(F32).reshape(nblocks, BLOCK, heads_local, HEAD_DIM)
    scaled = value_wide * step_length.reshape(nblocks, BLOCK, heads_local)[..., None]
    in_blocks = in_mat.reshape(nblocks, BLOCK, groups_local, STATE)
    in_head = jnp.repeat(in_blocks.astype(F32), head_ratio, axis=2)
    block_logs = running[:, -1]
    to_end = jnp.exp(block_logs[:, None, :] - running)
    block_state = jnp.einsum("bjhn,bjh,bjhp->bhpn", in_head, to_end, scaled)
    carried = jnp.zeros((heads_local, HEAD_DIM, STATE), F32)
    for b in range(nblocks):
        carried = carried * jnp.exp(block_logs[b])[:, None, None] + block_state[b]
    gathered_states = states_gathered(jnp.sum(block_logs, axis=0), carried)

    model_width = second_token_rows.shape[1]
    local_experts = routed_gate_weight.shape[0]
    ep_count = lax.axis_size("ep")
    experts = local_experts * ep_count
    tp_place = lax.axis_index("tp").astype(jnp.int32)
    at = tp_place.reshape(1)
    y = tp_place // SIDE
    columns = routed_down_weight.shape[2]
    share = model_width // SIDE
    outgoing, normed = dispatch(
        at, routed_expert_index.T, second_token_rows, expert_norm_scale, ep_count
    )
    arrived = lax.all_to_all(
        outgoing.reshape(ep_count, PADDED, share), "ep", split_axis=0, concat_axis=0, tiled=True
    )
    arrived = arrived.reshape(ep_count * PADDED, share)

    part_ff = routed_gate_weight.shape[2]
    tall = routed_down_weight.reshape(local_experts, SIDE * SIDE, part_ff, columns)
    tall = jnp.swapaxes(tall, 1, 2).reshape(local_experts, part_ff, model_width)
    both = jnp.concatenate(
        [jnp.swapaxes(routed_gate_weight, 1, 2), jnp.swapaxes(routed_up_weight, 1, 2), tall], axis=1
    )
    weights = [lax.dynamic_index_in_dim(both, y // 2, 0, False)]
    for by in (1, SIDE - 1, 2):
        goes = lax.dynamic_index_in_dim(both, ((y + by) % SIDE) // 2, 0, False)
        weights.append(shifted_down(goes, by))

    rows_local = second_token_rows.shape[0]
    tokens = jnp.broadcast_to(arrived[None], (SIDE,) + arrived.shape)
    tokens = along(tokens, ROW_GROUPS)
    hidden = shown_to_row(expert_hidden(tokens, weights))
    result = along(expert_down(at, hidden, weights), COLUMN_GROUPS)
    result = jnp.swapaxes(result.reshape(SIDE, ep_count, PADDED, columns), 0, 1)
    result = result.reshape(ep_count, SIDE * PADDED, columns)
    returned = lax.all_to_all(result, "ep", split_axis=0, concat_axis=0, tiled=True)
    returned = returned.reshape(ep_count * SIDE * PADDED, columns)

    shared_hidden = (
        jax.nn.silu(jnp.dot(normed, shared_gate_weight, preferred_element_type=F32))
        * jnp.dot(normed, shared_up_weight, preferred_element_type=F32)
    ).astype(BF16)
    flat = running.reshape(length, heads_local)
    payload = late_mixer(
        lax.axis_index("ep").astype(jnp.int32).reshape(1),
        gathered_states,
        values,
        in_mat,
        out_mat,
        flat,
        flat.T,
        step_length.T,
        output_gate_input,
        jnp.repeat(head_skip_scale, HEAD_DIM)[None, :],
        mixer_norm_scale[None, :],
        block_state[0].reshape(heads_local * HEAD_DIM, STATE),
        shared_hidden,
    )
    gathered = lax.all_gather(payload, "tp")
    mixer_output, shared_result = last_products(
        gathered, mixer_output_weight, shared_down_weight, rows_local
    )

    place, weight = places(routed_expert_index.T, routed_expert_weight.T, experts)
    by_owner = place.reshape(ep_count, local_experts, rows_local)
    halves = jnp.stack([slot_numbers(0), slot_numbers(1)])
    taken = by_owner[:, :, None, None, :] == halves[None, None, :, :, None]
    weight = weight.reshape(ep_count, local_experts, 1, 1, rows_local)
    weight_high = high(weight)
    contract = (((0,), (0,)), ((), ()))
    routed_sum = shared_result
    for part in (weight_high, weight - weight_high):
        spread_part = jnp.where(taken, part, 0.0).astype(BF16).reshape(-1, rows_local)
        routed_sum = routed_sum + lax.dot_general(
            spread_part, returned, contract, preferred_element_type=F32
        )
    routed_out = routed_sum.astype(BF16)
    return (mixer_output, routed_out)


def solution(mesh):
    return jax.shard_map(
        step,
        mesh=mesh,
        in_specs=(
            P("ep", "tp"),
            P("ep", "tp"),
            P("ep", "tp"),
            P("ep", "tp"),
            P("ep", "tp"),
            P("ep", "tp"),
            P("tp"),
            P("tp"),
            P(None, "tp"),
            P(None, "tp"),
            P(None, "tp"),
            P("tp"),
            P(None, "tp"),
            P("ep", None),
            P(),
            P("ep", None),
            P("ep", None),
            P("ep", None, "tp"),
            P("ep", None, "tp"),
            P("ep", None, "tp"),
            P(None, "tp"),
            P(None, "tp"),
            P(None, "tp"),
        ),
        out_specs=(P("ep", "tp"), P("ep", "tp")),
        check_vma=False,
    )
```
